32 devices in a mesh: grp: 2 (over x), ep: 8 (over z, y), tp: 2 (over core).
Axes of the slice: x: 2, y: 2, z: 4, core: 2. Of those that a mesh axis runs over, the one named last changes fastest.
Arguments:
- tokens: bfloat16 [2304, 2048], P(('grp', 'ep')), parts along dimension 0, may hold values from -6 to 6
- norm_gain: bfloat16 [2048], replicated, may hold values from 0.099609375 to 1.8984375
- chosen_rows: int32 [16, 144], P('grp', 'ep'), parts along dimension 0, may hold values from 0 to 1151, as said below
- route_weights: float32 [16, 144], P('grp', 'ep'), parts along dimension 0, may hold values from 0.2 to 1
- gate_weight: bfloat16 [8, 2048, 1536], P('ep', None, 'tp'), may hold values from -0.125 to 0.125
- up_weight: bfloat16 [8, 2048, 1536], P('ep', None, 'tp'), may hold values from -0.125 to 0.125
- down_weight: bfloat16 [8, 1536, 2048], P('ep', 'tp'), may hold values from -0.15625 to 0.15625
Outputs:
- mixed: bfloat16 [2304, 2048], P(('grp', 'ep', 'tp')), parts along dimension 0
The draws below stay inside these ranges and needn't reach their ends.
There are 2 independent parts, one for each index of `grp`. The reference program is written for one: setup_inputs(seed, part) draws one part's arguments, and reference() takes and returns one part's arrays. A program takes and returns all parts, laid end to end along the dimension named above; an argument that names none is the same for every part. Nothing has to cross between parts.
Inputs may be any that keep to these rules, and one draw needn't show every extreme that they name: `chosen_rows`: the columns come in blocks of 18, one block for each index of ep's 144 tokens in order. In every row the first half of a block names distinct tokens of the first half of that block's tokens, and its second half distinct tokens of the second half.
All inputs are finite; a program needn't handle non-finite values.
Results may differ from the reference program's by a relative error of at most 0.01.
Values may be sent and summed in bfloat16 or wider, within the bound.
A program may use at most 128 MiB of HBM per device.

```python
import jax
import jax.numpy as jnp
from jax import lax

D = 2048
FF = 1536
TOK_DEV = 144
EXPERTS = 8
TOKENS = 1152
SLOTS = 18
CAP = 144
N_TP = 2


def draw_chosen_rows(key, part):
    sources = CAP // SLOTS
    half_rows = TOK_DEV // 2
    half_slots = SLOTS // 2
    scores = jax.random.randint(jax.random.fold_in(key, 11), (EXPERTS, sources, 2, half_rows), 0, 1048576)
    scores = scores * half_rows + jnp.arange(half_rows, dtype=jnp.int32)
    order = jnp.argsort(scores, axis=-1, stable=True)[..., :half_slots].astype(jnp.int32)
    source_ids = jnp.arange(sources, dtype=jnp.int32)[None, :, None, None] * TOK_DEV
    half_ids = jnp.arange(2, dtype=jnp.int32)[None, None, :, None] * half_rows
    rows = order + source_ids + half_ids
    return rows.reshape(EXPERTS, CAP).astype(jnp.int32)


def steps_of(rng, extent, shards, low, largest):
    loudness, own = 1.0, jax.random.fold_in(rng, 6)
    for dim, parts in shards:
        heights = jnp.exp(jax.random.uniform(jax.random.fold_in(own, dim), (parts,), jnp.float32, low / len(shards), largest / len(shards)))
        loudness = loudness * jnp.repeat(heights, extent[dim] // parts).reshape([-1 if axis == dim else 1 for axis in range(len(extent))])
    return loudness


def noise(rng, shape, deviation, most, shards=(), kind=jnp.bfloat16):
    result = deviation * jax.random.normal(rng, shape, jnp.float32)
    if shards:
        result = result * steps_of(rng, shape, shards, -0.22, 0.18)
    return jnp.clip(result, -most, most).astype(kind)


def setup_inputs(seed: int = 0, part: int = 0) -> dict:
    arg_keys = jax.random.split(jax.random.key(seed), 8)
    part_splits = jax.random.split(jax.random.fold_in(arg_keys[7], part), 8)
    return {
        "tokens": noise(part_splits[0], (TOKENS, D), 1.0, 6.0, ((0, 8),)),
        "norm_gain": jnp.clip(1.0 + 0.18 * jax.random.normal(arg_keys[1], (D,), jnp.float32), 0.099609375, 1.8984375).astype(jnp.bfloat16),
        "chosen_rows": draw_chosen_rows(jax.random.fold_in(jax.random.fold_in(arg_keys[7], part), 71), part),
        "route_weights": jnp.clip(0.2 + 0.8 * jax.random.uniform(part_splits[3], (EXPERTS, CAP), jnp.float32) ** steps_of(part_splits[3], (EXPERTS, CAP), ((1, 8),), -0.2, 0.2), 0.2, 1.0),
        "gate_weight": noise(arg_keys[4], (EXPERTS, D, FF), D ** -0.5, 0.125, ((0, 8), (2, 2))),
        "up_weight": noise(arg_keys[5], (EXPERTS, D, FF), D ** -0.5, 0.125, ((0, 8), (2, 2))),
        "down_weight": noise(arg_keys[6], (EXPERTS, FF, D), FF ** -0.5, 0.15625, ((0, 8), (1, 2))),
    }


def reference(tokens, norm_gain, chosen_rows, route_weights, gate_weight, up_weight, down_weight):
    values = tokens.astype(jnp.float32)
    scale = lax.rsqrt(lax.optimization_barrier(jnp.mean(values * values, axis=-1, keepdims=True)) + 1e-06)
    normed = (values * scale * norm_gain.astype(jnp.float32)).astype(jnp.bfloat16)
    half_ff = FF // N_TP

    def one_expert(total, inputs):
        expert_rows, expert_weights, w_gate, w_up, w_down = inputs
        expert_in = normed[expert_rows]
        gate_proj = jnp.dot(expert_in, w_gate, preferred_element_type=jnp.float32)
        up_proj = jnp.dot(expert_in, w_up, preferred_element_type=jnp.float32)
        hidden = (jax.nn.silu(gate_proj) * up_proj).astype(jnp.bfloat16)
        summed = jnp.zeros((expert_rows.shape[0], D), jnp.float32)
        for part_id in range(N_TP):
            partial_out = jnp.dot(hidden[:, part_id * half_ff:(part_id + 1) * half_ff], w_down[part_id * half_ff:(part_id + 1) * half_ff], preferred_element_type=jnp.float32).astype(jnp.bfloat16)
            partial_out = lax.optimization_barrier(partial_out)
            summed = summed + partial_out.astype(jnp.float32)
        expert_out = summed.astype(jnp.bfloat16)
        total = total.at[expert_rows].add(expert_weights[:, None] * expert_out.astype(jnp.float32))
        return (total, None)
    start_total = jnp.zeros((TOKENS, D), jnp.float32)
    total, unused = lax.scan(one_expert, start_total, (chosen_rows.astype(jnp.int32), route_weights, gate_weight, up_weight, down_weight))
    return total.astype(jnp.bfloat16)
```

```python
import functools

import jax
import jax.numpy as jnp
from jax import lax
from jax.experimental import pallas as pl
from jax.experimental.pallas import tpu as pltpu
from jax.sharding import PartitionSpec as P

MESH = pl.DeviceIdType.MESH
LANES = 128
SUB = 8
GROUP = 8


def loop(count, body):
    if count == 1:
        body(0)
    else:
        lax.fori_loop(0, count, lambda i, carry: (body(i), carry)[1], 0)


def kernel(
    n,
    tokens,
    gain,
    chosen,
    route,
    gate_w,
    up_w,
    down_w,
    mixed,
    tok,
    wg,
    wu,
    wd,
    normed,
    out_x,
    in_x,
    sib_x,
    flat,
    x_cols,
    gate_acc,
    up_acc,
    hidden,
    p_send,
    p_recv,
    p_own,
    c_send,
    c_recv,
    g_rows,
    w_rows,
    r_cols,
    load_sem,
    d_send,
    d_recv,
    f_send,
    f_recv,
    q_send,
    q_recv,
    b_send,
    b_recv,
):
    chunks = out_x.shape[0]
    half_rows, width = tok.shape
    experts, slots = chosen.shape
    half = slots // 2
    rows = experts * half
    block = GROUP * half
    blocks = rows // block
    cols = width // chunks
    me = lax.axis_index("ep")
    core = lax.axis_index("tp")
    sib = {"tp": 1 - core}

    def peer(i):
        return lax.rem(me + i, n)

    barrier = pltpu.get_barrier_semaphore()
    pl.semaphore_signal(barrier, inc=1, device_id=sib, device_id_type=MESH)
    lax.fori_loop(
        1,
        n,
        lambda i, c: (
            pl.semaphore_signal(barrier, inc=1, device_id={"ep": peer(i)}, device_id_type=MESH),
            c,
        )[1],
        0,
    )
    base = pl.multiple_of(core * half_rows, 8)
    load_tok = pltpu.make_async_copy(tokens.at[pl.ds(base, half_rows)], tok, load_sem.at[0])
    load_tok.start()
    loads = [
        pltpu.make_async_copy(src.at[0], dst, load_sem.at[i + 1])
        for i, (src, dst) in enumerate(((gate_w, wg), (up_w, wu), (down_w, wd)))
    ]
    for load in loads:
        load.start()
    load_tok.wait()

    g = gain[...].astype(jnp.float32)
    values = tok[...].astype(jnp.float32)
    scale = lax.rsqrt(jnp.mean(values * values, axis=-1, keepdims=True) + 1e-06)
    normed[...] = (values * scale * g).astype(jnp.bfloat16)

    first = me * (2 * half_rows) + core * half_rows
    picked = (chosen[...] - first).astype(jnp.float32).T
    weight = route[...].T
    lane = lax.broadcasted_iota(jnp.int32, (half, half_rows), 1).astype(jnp.float32)
    for e in range(experts):
        pair = [picked[h * half : (h + 1) * half, e : e + 1] for h in range(2)]
        row = jnp.where(core == 0, pair[0], pair[1])
        pair = [weight[h * half : (h + 1) * half, e : e + 1] for h in range(2)]
        share = jnp.where(core == 0, pair[0], pair[1])
        here = lane == row
        g_rows[e * half : (e + 1) * half, :] = jnp.where(here, 1.0, 0.0)
        w_rows[e * half : (e + 1) * half, :] = jnp.where(here, share, 0.0)

    def start_of(b):
        return b * block if isinstance(b, int) else pl.multiple_of(b * block, 8)

    def pack(value, ref, j, b):
        for s in range(SUB):
            flat[pl.ds(s, block, stride=SUB), :] = value[:, s * LANES : (s + 1) * LANES]
        ref[j, pl.ds(b * block, block)] = (
            flat[: block * SUB, :].reshape(block, SUB, LANES).astype(jnp.bfloat16)
        )

    def gather(j):
        def one(b):
            hot = g_rows[pl.ds(start_of(b), block), :].astype(jnp.bfloat16)
            got = jnp.dot(
                hot, normed[:, j * cols : (j + 1) * cols], preferred_element_type=jnp.float32
            )
            pack(got, out_x, j, b)

        loop(blocks, one)

    def mine(ref, j, e):
        return ref.at[j, pl.ds(e * half, half)]

    def exchange(src, dst, j, send_sem, recv_sem):
        def one(i, c):
            e = peer(i)
            pltpu.make_async_remote_copy(
                src_ref=mine(src, j, e),
                dst_ref=mine(dst, j, me),
                send_sem=send_sem.at[j],
                recv_sem=recv_sem.at[j],
                device_id={"ep": e},
                device_id_type=MESH,
            ).start()
            return c

        lax.fori_loop(1, n, one, 0)
        for r in range(half):
            dst[j, me * half + r] = src[j, me * half + r]

    def all_of(src, dst, j, send_sem, recv_sem):
        part = pl.ds(0, (n - 1) * half)
        return pltpu.make_async_remote_copy(
            src_ref=src.at[j, part],
            dst_ref=dst.at[j, part],
            send_sem=send_sem.at[j],
            recv_sem=recv_sem.at[j],
            device_id=sib,
            device_id_type=MESH,
        )

    def to_sib(src, dst, j, send_sem, recv_sem):
        return pltpu.make_async_remote_copy(
            src_ref=src.at[j],
            dst_ref=dst.at[j],
            send_sem=send_sem.at[j],
            recv_sem=recv_sem.at[j],
            device_id=sib,
            device_id_type=MESH,
        )

    gather(0)
    pl.semaphore_wait(barrier, n)
    exchange(out_x, in_x, 0, d_send, d_recv)
    for j in range(1, chunks):
        gather(j)
        exchange(out_x, in_x, j, d_send, d_recv)

    for j in range(chunks):
        all_of(out_x, in_x, j, d_send, d_recv).wait_recv()
        to_sib(in_x, sib_x, j, f_send, f_recv).start()
    for load in loads:
        load.wait()
    for j in range(chunks):
        to_sib(in_x, sib_x, j, f_send, f_recv).wait_recv()

        def project(b):
            for h, ref in enumerate((in_x, sib_x)):
                got = ref[j, pl.ds(b * block, block)].astype(jnp.float32)
                flat[pl.ds(h * block * SUB, block * SUB), :] = got.reshape(block * SUB, LANES)
            for s in range(SUB):
                x_cols[:, s * LANES : (s + 1) * LANES] = flat[
                    pl.ds(s, 2 * block, stride=SUB), :
                ].astype(jnp.bfloat16)
            x = x_cols[...]
            depth = slice(j * cols, (j + 1) * cols)
            gate = jnp.dot(x, wg[depth, :], preferred_element_type=jnp.float32)
            up = jnp.dot(x, wu[depth, :], preferred_element_type=jnp.float32)
            if j > 0:
                gate = gate + gate_acc[b]
                up = up + up_acc[b]
            if j < chunks - 1:
                gate_acc[b] = gate
                up_acc[b] = up
            else:
                hidden[b] = (gate / (1.0 + jnp.exp(-gate)) * up).astype(jnp.bfloat16)

        loop(blocks, project)

    for j in range(chunks):

        def down(b):
            part = jnp.dot(
                hidden[b], wd[:, j * cols : (j + 1) * cols], preferred_element_type=jnp.float32
            )
            p_own[j, b] = part[:block].astype(jnp.bfloat16)
            p_send[j, b] = part[block:].astype(jnp.bfloat16)

        loop(blocks, down)
        to_sib(p_send, p_recv, j, q_send, q_recv).start()

    for j in range(chunks):
        to_sib(p_send, p_recv, j, q_send, q_recv).wait_recv()

        def combine(b):
            total = p_own[j, b].astype(jnp.float32) + p_recv[j, b].astype(jnp.float32)
            pack(total, c_send, j, b)

        loop(blocks, combine)
        exchange(c_send, c_recv, j, b_send, b_recv)

    spread = w_rows[...].T
    high = spread.astype(jnp.bfloat16)
    low = (spread - high.astype(jnp.float32)).astype(jnp.bfloat16)
    for j in range(chunks):
        all_of(c_send, c_recv, j, b_send, b_recv).wait_recv()

        def unpack(b):
            got = c_recv[j, pl.ds(b * block, block)].astype(jnp.float32)
            flat[: block * SUB, :] = got.reshape(block * SUB, LANES)
            at = start_of(b)
            for s in range(SUB):
                r_cols[pl.ds(at, block), s * LANES : (s + 1) * LANES] = flat[
                    pl.ds(s, block, stride=SUB), :
                ]

        loop(blocks, unpack)
        res = r_cols[...].astype(jnp.bfloat16)
        total = jnp.dot(high, res, preferred_element_type=jnp.float32)
        total = total + jnp.dot(low, res, preferred_element_type=jnp.float32)
        mixed[:, j * cols : (j + 1) * cols] = total.astype(jnp.bfloat16)

    for j in range(chunks):
        all_of(out_x, in_x, j, d_send, d_recv).wait_send()
        to_sib(in_x, sib_x, j, f_send, f_recv).wait_send()
        to_sib(p_send, p_recv, j, q_send, q_recv).wait_send()
        all_of(c_send, c_recv, j, b_send, b_recv).wait_send()


def local(n, tokens, norm_gain, chosen_rows, route_weights, gate_weight, up_weight, down_weight):
    tok_rows, width = tokens.shape
    half_rows = tok_rows // 2
    experts, slots = chosen_rows.shape
    half = slots // 2
    rows = experts * half
    block = GROUP * half
    blocks = rows // block
    ff = gate_weight.shape[2]
    chunks = width // (LANES * SUB)
    cols = width // chunks
    bf16, f32 = jnp.bfloat16, jnp.float32
    packed = pltpu.VMEM((chunks, rows, SUB, LANES), bf16)
    partial = pltpu.VMEM((chunks, blocks, block, cols), bf16)
    vmem = pl.BlockSpec(memory_space=pltpu.VMEM)
    hbm = pl.BlockSpec(memory_space=pl.ANY)
    return pl.pallas_call(
        functools.partial(kernel, n),
        out_shape=jax.ShapeDtypeStruct((half_rows, width), bf16),
        in_specs=[hbm, vmem, vmem, vmem, hbm, hbm, hbm],
        out_specs=vmem,
        scratch_shapes=[
            pltpu.VMEM((half_rows, width), bf16),
            pltpu.VMEM(gate_weight.shape[1:], bf16),
            pltpu.VMEM(up_weight.shape[1:], bf16),
            pltpu.VMEM(down_weight.shape[1:], bf16),
            pltpu.VMEM((half_rows, width), bf16),
            packed,
            packed,
            packed,
            pltpu.VMEM((2 * block * SUB, LANES), f32),
            pltpu.VMEM((2 * block, cols), bf16),
            pltpu.VMEM((blocks, 2 * block, ff), f32),
            pltpu.VMEM((blocks, 2 * block, ff), f32),
            pltpu.VMEM((blocks, 2 * block, ff), bf16),
            partial,
            partial,
            partial,
            packed,
            packed,
            pltpu.VMEM((rows, half_rows), f32),
            pltpu.VMEM((rows, half_rows), f32),
            pltpu.VMEM((rows, cols), f32),
            pltpu.SemaphoreType.DMA((4,)),
        ]
        + [pltpu.SemaphoreType.DMA((chunks,))] * 8,
        compiler_params=pltpu.CompilerParams(
            collective_id=0, has_side_effects=True, vmem_limit_bytes=60 * 1024 * 1024
        ),
    )(
        tokens,
        norm_gain.reshape(1, width),
        chosen_rows,
        route_weights,
        gate_weight,
        up_weight,
        down_weight,
    )


def solution(mesh):
    return jax.shard_map(
        functools.partial(local, mesh.shape["ep"]),
        mesh=mesh,
        in_specs=(
            P(("grp", "ep"), None),
            P(),
            P("grp", "ep"),
            P("grp", "ep"),
            P("ep", None, "tp"),
            P("ep", None, "tp"),
            P("ep", "tp", None),
        ),
        out_specs=P(("grp", "ep", "tp"), None),
        check_vma=False,
    )
```

```python
import functools

import jax
import jax.numpy as jnp
from jax import lax
from jax.experimental import pallas as pl
from jax.experimental.pallas import tpu as pltpu
from jax.sharding import PartitionSpec as P

MESH = pl.DeviceIdType.MESH
LANES = 128
SUB = 8
GROUP = 8
VMEM_BYTES = 67043328


def loop(count, body):
    if count == 1:
        body(0)
    else:
        lax.fori_loop(0, count, lambda i, carry: (body(i), carry)[1], 0)


def kernel(
    n,
    tokens,
    gain_h,
    chosen_h,
    route_h,
    gate_w,
    up_w,
    down_w,
    mixed,
    tok,
    gain,
    chosen,
    route,
    wg,
    wu,
    wd,
    normed,
    out_x,
    in_x,
    sib_x,
    flat,
    x_cols,
    gate_acc,
    up_acc,
    hidden,
    p_send,
    p_recv,
    p_own,
    c_send,
    c_recv,
    g_rows,
    w_rows,
    r_cols,
    load_sem,
    d_send,
    d_recv,
    f_send,
    f_recv,
    q_send,
    q_recv,
    b_send,
    b_recv,
):
    chunks = out_x.shape[0]
    half_rows, width = tok.shape
    experts, slots = chosen.shape
    half = slots // 2
    rows = experts * half
    block = GROUP * half
    blocks = rows // block
    cols = width // chunks
    me = lax.axis_index("ep")
    core = lax.axis_index("tp")
    sib = {"tp": 1 - core}

    def peer(i):
        return lax.rem(me + i, n)

    barrier = pltpu.get_barrier_semaphore()
    pl.semaphore_signal(barrier, inc=1, device_id=sib, device_id_type=MESH)
    lax.fori_loop(
        1,
        n,
        lambda i, c: (
            pl.semaphore_signal(barrier, inc=1, device_id={"ep": peer(i)}, device_id_type=MESH),
            c,
        )[1],
        0,
    )
    base = pl.multiple_of(core * half_rows, 8)
    load_tok = pltpu.make_async_copy(tokens.at[pl.ds(base, half_rows)], tok, load_sem.at[0])
    load_tok.start()
    small = [
        pltpu.make_async_copy(src, dst, load_sem.at[i + 4])
        for i, (src, dst) in enumerate(((gain_h, gain), (chosen_h, chosen), (route_h, route)))
    ]
    for load in small:
        load.start()
    loads = [
        pltpu.make_async_copy(src.at[0], dst, load_sem.at[i + 1])
        for i, (src, dst) in enumerate(((gate_w, wg), (up_w, wu), (down_w, wd)))
    ]
    for load in loads:
        load.start()
    for load in small:
        load.wait()
    load_tok.wait()

    g = gain[...].astype(jnp.float32).reshape(1, width)
    values = tok[...].astype(jnp.float32)
    scale = lax.rsqrt(jnp.mean(values * values, axis=-1, keepdims=True) + 1e-06)
    normed[...] = (values * scale * g).astype(jnp.bfloat16)

    first = me * (2 * half_rows) + core * half_rows
    picked = (chosen[...] - first).astype(jnp.float32).T
    weight = route[...].T
    lane = lax.broadcasted_iota(jnp.int32, (half, half_rows), 1).astype(jnp.float32)
    for e in range(experts):
        pair = [picked[h * half : (h + 1) * half, e : e + 1] for h in range(2)]
        row = jnp.where(core == 0, pair[0], pair[1])
        pair = [weight[h * half : (h + 1) * half, e : e + 1] for h in range(2)]
        share = jnp.where(core == 0, pair[0], pair[1])
        here = lane == row
        g_rows[e * half : (e + 1) * half, :] = jnp.where(here, 1.0, 0.0)
        w_rows[e * half : (e + 1) * half, :] = jnp.where(here, share, 0.0)

    def start_of(b):
        return b * block if isinstance(b, int) else pl.multiple_of(b * block, 8)

    def pack(value, ref, j, b):
        for s in range(SUB):
            flat[pl.ds(s, block, stride=SUB), :] = value[:, s * LANES : (s + 1) * LANES]
        ref[j, pl.ds(b * block, block)] = (
            flat[: block * SUB, :].reshape(block, SUB, LANES).astype(jnp.bfloat16)
        )

    def gather(j):
        def one(b):
            hot = g_rows[pl.ds(start_of(b), block), :].astype(jnp.bfloat16)
            got = jnp.dot(
                hot, normed[:, j * cols : (j + 1) * cols], preferred_element_type=jnp.float32
            )
            pack(got, out_x, j, b)

        loop(blocks, one)

    def mine(ref, j, e):
        return ref.at[j, pl.ds(e * half, half)]

    def exchange(src, dst, j, send_sem, recv_sem):
        def one(i, c):
            e = peer(i)
            pltpu.make_async_remote_copy(
                src_ref=mine(src, j, e),
                dst_ref=mine(dst, j, me),
                send_sem=send_sem.at[j],
                recv_sem=recv_sem.at[j],
                device_id={"ep": e},
                device_id_type=MESH,
            ).start()
            return c

        lax.fori_loop(1, n, one, 0)
        for r in range(half):
            dst[j, me * half + r] = src[j, me * half + r]

    def all_of(src, dst, j, send_sem, recv_sem):
        part = pl.ds(0, (n - 1) * half)
        return pltpu.make_async_remote_copy(
            src_ref=src.at[j, part],
            dst_ref=dst.at[j, part],
            send_sem=send_sem.at[j],
            recv_sem=recv_sem.at[j],
            device_id=sib,
            device_id_type=MESH,
        )

    def to_sib(src, dst, j, send_sem, recv_sem):
        return pltpu.make_async_remote_copy(
            src_ref=src.at[j],
            dst_ref=dst.at[j],
            send_sem=send_sem.at[j],
            recv_sem=recv_sem.at[j],
            device_id=sib,
            device_id_type=MESH,
        )

    gather(0)
    pl.semaphore_wait(barrier, n)
    exchange(out_x, in_x, 0, d_send, d_recv)
    for j in range(1, chunks):
        gather(j)
        exchange(out_x, in_x, j, d_send, d_recv)

    for j in range(chunks):
        all_of(out_x, in_x, j, d_send, d_recv).wait_recv()
        to_sib(in_x, sib_x, j, f_send, f_recv).start()
    for load in loads:
        load.wait()
    for j in range(chunks):
        to_sib(in_x, sib_x, j, f_send, f_recv).wait_recv()

        def project(b):
            for h, ref in enumerate((in_x, sib_x)):
                got = ref[j, pl.ds(b * block, block)].astype(jnp.float32)
                flat[pl.ds(h * block * SUB, block * SUB), :] = got.reshape(block * SUB, LANES)
            for s in range(SUB):
                x_cols[:, s * LANES : (s + 1) * LANES] = flat[
                    pl.ds(s, 2 * block, stride=SUB), :
                ].astype(jnp.bfloat16)
            x = x_cols[...]
            depth = slice(j * cols, (j + 1) * cols)
            gate = jnp.dot(x, wg[depth, :], preferred_element_type=jnp.float32)
            up = jnp.dot(x, wu[depth, :], preferred_element_type=jnp.float32)
            if j > 0:
                gate = gate + gate_acc[b]
                up = up + up_acc[b]
            if j < chunks - 1:
                gate_acc[b] = gate
                up_acc[b] = up
            else:
                hidden[b] = (gate / (1.0 + jnp.exp(-gate)) * up).astype(jnp.bfloat16)

        loop(blocks, project)

    for j in range(chunks):

        def down(b):
            part = jnp.dot(
                hidden[b], wd[:, j * cols : (j + 1) * cols], preferred_element_type=jnp.float32
            )
            p_own[j, b] = part[:block].astype(jnp.bfloat16)
            p_send[j, b] = part[block:].astype(jnp.bfloat16)

        loop(blocks, down)
        to_sib(p_send, p_recv, j, q_send, q_recv).start()

    for j in range(chunks):
        to_sib(p_send, p_recv, j, q_send, q_recv).wait_recv()

        def combine(b):
            total = p_own[j, b].astype(jnp.float32) + p_recv[j, b].astype(jnp.float32)
            pack(total, c_send, j, b)

        loop(blocks, combine)
        exchange(c_send, c_recv, j, b_send, b_recv)

    spread = w_rows[...].T
    high = spread.astype(jnp.bfloat16)
    low = (spread - high.astype(jnp.float32)).astype(jnp.bfloat16)
    for j in range(chunks):
        all_of(c_send, c_recv, j, b_send, b_recv).wait_recv()

        def unpack(b):
            got = c_recv[j, pl.ds(b * block, block)].astype(jnp.float32)
            flat[: block * SUB, :] = got.reshape(block * SUB, LANES)
            at = start_of(b)
            for s in range(SUB):
                r_cols[pl.ds(at, block), s * LANES : (s + 1) * LANES] = flat[
                    pl.ds(s, block, stride=SUB), :
                ]

        loop(blocks, unpack)
        res = r_cols[...].astype(jnp.bfloat16)
        total = jnp.dot(high, res, preferred_element_type=jnp.float32)
        total = total + jnp.dot(low, res, preferred_element_type=jnp.float32)
        mixed[:, j * cols : (j + 1) * cols] = total.astype(jnp.bfloat16)

    for j in range(chunks):
        all_of(out_x, in_x, j, d_send, d_recv).wait_send()
        to_sib(in_x, sib_x, j, f_send, f_recv).wait_send()
        to_sib(p_send, p_recv, j, q_send, q_recv).wait_send()
        all_of(c_send, c_recv, j, b_send, b_recv).wait_send()


def local(n, tokens, norm_gain, chosen_rows, route_weights, gate_weight, up_weight, down_weight):
    tok_rows, width = tokens.shape
    half_rows = tok_rows // 2
    experts, slots = chosen_rows.shape
    half = slots // 2
    rows = experts * half
    block = GROUP * half
    blocks = rows // block
    ff = gate_weight.shape[2]
    chunks = width // (LANES * SUB)
    cols = width // chunks
    bf16, f32 = jnp.bfloat16, jnp.float32
    packed = pltpu.VMEM((chunks, rows, SUB, LANES), bf16)
    partial = pltpu.VMEM((chunks, blocks, block, cols), bf16)
    vmem = pl.BlockSpec(memory_space=pltpu.VMEM)
    hbm = pl.BlockSpec(memory_space=pltpu.HBM)
    scratch = [
        pltpu.VMEM((half_rows, width), bf16),
        pltpu.VMEM(norm_gain.shape, norm_gain.dtype),
        pltpu.VMEM(chosen_rows.shape, chosen_rows.dtype),
        pltpu.VMEM(route_weights.shape, route_weights.dtype),
        pltpu.VMEM(gate_weight.shape[1:], bf16),
        pltpu.VMEM(up_weight.shape[1:], bf16),
        pltpu.VMEM(down_weight.shape[1:], bf16),
        pltpu.VMEM((half_rows, width), bf16),
        packed,
        packed,
        packed,
        pltpu.VMEM((2 * block * SUB, LANES), f32),
        pltpu.VMEM((2 * block, cols), bf16),
        pltpu.VMEM((blocks, 2 * block, ff), f32),
        pltpu.VMEM((blocks, 2 * block, ff), f32),
        pltpu.VMEM((blocks, 2 * block, ff), bf16),
        partial,
        partial,
        partial,
        packed,
        packed,
        pltpu.VMEM((rows, half_rows), f32),
        pltpu.VMEM((rows, half_rows), f32),
        pltpu.VMEM((rows, cols), f32),
    ]
    limit = VMEM_BYTES - half_rows * width * 2
    return pl.pallas_call(
        functools.partial(kernel, n),
        out_shape=jax.ShapeDtypeStruct((half_rows, width), bf16),
        in_specs=[hbm] * 7,
        out_specs=vmem,
        scratch_shapes=scratch
        + [pltpu.SemaphoreType.DMA((7,))]
        + [pltpu.SemaphoreType.DMA((chunks,))] * 8,
        compiler_params=pltpu.CompilerParams(
            collective_id=0, has_side_effects=True, vmem_limit_bytes=limit
        ),
    )(
        tokens,
        norm_gain,
        chosen_rows,
        route_weights,
        gate_weight,
        up_weight,
        down_weight,
    )


def solution(mesh):
    return jax.shard_map(
        functools.partial(local, mesh.shape["ep"]),
        mesh=mesh,
        in_specs=(
            P(("grp", "ep"), None),
            P(),
            P("grp", "ep"),
            P("grp", "ep"),
            P("ep", None, "tp"),
            P("ep", None, "tp"),
            P("ep", "tp", None),
        ),
        out_specs=P(("grp", "ep", "tp"), None),
        check_vma=False,
    )
```

```python
import functools

import jax
import jax.numpy as jnp
from jax import lax
from jax.experimental import pallas as pl
from jax.experimental.pallas import tpu as pltpu
from jax.sharding import PartitionSpec as P

MESH = pl.DeviceIdType.MESH
LANES = 128
SUB = 8
GROUP = 8
VMEM_BYTES = 67043328


def loop(count, body):
    if count == 1:
        body(0)
    else:
        lax.fori_loop(0, count, lambda i, carry: (body(i), carry)[1], 0)


def kernel(
    n,
    tokens,
    gain_h,
    chosen_h,
    route_h,
    gate_w,
    up_w,
    down_w,
    mixed,
    tok,
    gain,
    chosen,
    route,
    wg,
    wu,
    wd,
    normed,
    out_x,
    in_x,
    sib_x,
    flat,
    x_cols,
    gate_acc,
    up_acc,
    hidden,
    p_send,
    p_recv,
    p_own,
    c_send,
    c_recv,
    g_rows,
    w_rows,
    r_cols,
    load_sem,
    d_send,
    d_recv,
    f_send,
    f_recv,
    q_send,
    q_recv,
    b_send,
    b_recv,
):
    chunks = out_x.shape[0]
    half_rows, width = tok.shape
    experts, slots = chosen.shape
    half = slots // 2
    rows = experts * half
    block = GROUP * half
    blocks = rows // block
    cols = width // chunks
    me = lax.axis_index("ep")
    core = lax.axis_index("tp")
    sib = {"tp": 1 - core}

    def peer(i):
        return lax.rem(me + i, n)

    barrier = pltpu.get_barrier_semaphore()
    pl.semaphore_signal(barrier, inc=1, device_id=sib, device_id_type=MESH)
    lax.fori_loop(
        1,
        n,
        lambda i, c: (
            pl.semaphore_signal(barrier, inc=1, device_id={"ep": peer(i)}, device_id_type=MESH),
            c,
        )[1],
        0,
    )
    base = pl.multiple_of(core * half_rows, 8)
    load_tok = pltpu.make_async_copy(tokens.at[pl.ds(base, half_rows)], tok, load_sem.at[0])
    load_tok.start()
    small = [
        pltpu.make_async_copy(src, dst, load_sem.at[i + 4])
        for i, (src, dst) in enumerate(((gain_h, gain), (chosen_h, chosen), (route_h, route)))
    ]
    for load in small:
        load.start()
    loads = [
        pltpu.make_async_copy(src.at[0], dst, load_sem.at[i + 1])
        for i, (src, dst) in enumerate(((gate_w, wg), (up_w, wu), (down_w, wd)))
    ]
    for load in loads:
        load.start()
    for load in small:
        load.wait()
    load_tok.wait()

    g = gain[...].astype(jnp.float32).reshape(1, width)
    values = tok[...].astype(jnp.float32)
    scale = lax.rsqrt(jnp.mean(values * values, axis=-1, keepdims=True) + 1e-06)
    normed[...] = (values * scale * g).astype(jnp.bfloat16)

    first = me * (2 * half_rows) + core * half_rows
    picked = (chosen[...] - first).astype(jnp.float32).T
    weight = route[...].T
    lane = lax.broadcasted_iota(jnp.int32, (half, half_rows), 1).astype(jnp.float32)
    for e in range(experts):
        pair = [picked[h * half : (h + 1) * half, e : e + 1] for h in range(2)]
        row = jnp.where(core == 0, pair[0], pair[1])
        pair = [weight[h * half : (h + 1) * half, e : e + 1] for h in range(2)]
        share = jnp.where(core == 0, pair[0], pair[1])
        here = lane == row
        g_rows[e * half : (e + 1) * half, :] = jnp.where(here, 1.0, 0.0)
        w_rows[e * half : (e + 1) * half, :] = jnp.where(here, share, 0.0)

    def start_of(b):
        return b * block if isinstance(b, int) else pl.multiple_of(b * block, 8)

    def pack(value, ref, j, b):
        for s in range(SUB):
            flat[pl.ds(s, block, stride=SUB), :] = value[:, s * LANES : (s + 1) * LANES]
        ref[j, pl.ds(b * block, block)] = (
            flat[: block * SUB, :].reshape(block, SUB, LANES).astype(jnp.bfloat16)
        )

    def gather(j):
        def one(b):
            hot = g_rows[pl.ds(start_of(b), block), :].astype(jnp.bfloat16)
            got = jnp.dot(
                hot, normed[:, j * cols : (j + 1) * cols], preferred_element_type=jnp.float32
            )
            pack(got, out_x, j, b)

        loop(blocks, one)

    def mine(ref, j, e):
        return ref.at[j, pl.ds(e * half, half)]

    def exchange(src, dst, j, send_sem, recv_sem):
        def one(i, c):
            e = peer(i)
            pltpu.make_async_remote_copy(
                src_ref=mine(src, j, e),
                dst_ref=mine(dst, j, me),
                send_sem=send_sem.at[j],
                recv_sem=recv_sem.at[j],
                device_id={"ep": e},
                device_id_type=MESH,
            ).start()
            return c

        lax.fori_loop(1, n, one, 0)
        for r in range(half):
            dst[j, me * half + r] = src[j, me * half + r]

    def all_of(src, dst, j, send_sem, recv_sem):
        part = pl.ds(0, (n - 1) * half)
        return pltpu.make_async_remote_copy(
            src_ref=src.at[j, part],
            dst_ref=dst.at[j, part],
            send_sem=send_sem.at[j],
            recv_sem=recv_sem.at[j],
            device_id=sib,
            device_id_type=MESH,
        )

    def to_sib(src, dst, j, send_sem, recv_sem):
        return pltpu.make_async_remote_copy(
            src_ref=src.at[j],
            dst_ref=dst.at[j],
            send_sem=send_sem.at[j],
            recv_sem=recv_sem.at[j],
            device_id=sib,
            device_id_type=MESH,
        )

    gather(0)
    pl.semaphore_wait(barrier, n)
    exchange(out_x, in_x, 0, d_send, d_recv)
    for j in range(1, chunks):
        gather(j)
        exchange(out_x, in_x, j, d_send, d_recv)

    for j in range(chunks):
        all_of(out_x, in_x, j, d_send, d_recv).wait_recv()
        to_sib(in_x, sib_x, j, f_send, f_recv).start()
    for load in loads:
        load.wait()
    for j in range(chunks):
        to_sib(in_x, sib_x, j, f_send, f_recv).wait_recv()

        def project(b):
            for h, ref in enumerate((in_x, sib_x)):
                got = ref[j, pl.ds(b * block, block)].astype(jnp.float32)
                flat[pl.ds(h * block * SUB, block * SUB), :] = got.reshape(block * SUB, LANES)
            for s in range(SUB):
                x_cols[:, s * LANES : (s + 1) * LANES] = flat[
                    pl.ds(s, 2 * block, stride=SUB), :
                ].astype(jnp.bfloat16)
            x = x_cols[...]
            depth = slice(j * cols, (j + 1) * cols)
            gate = jnp.dot(x, wg[depth, :], preferred_element_type=jnp.float32)
            up = jnp.dot(x, wu[depth, :], preferred_element_type=jnp.float32)
            if j > 0:
                gate = gate + gate_acc[b]
                up = up + up_acc[b]
            if j < chunks - 1:
                gate_acc[b] = gate
                up_acc[b] = up
            else:
                hidden[b] = (gate / (1.0 + jnp.exp(-gate)) * up).astype(jnp.bfloat16)

        loop(blocks, project)

    for j in range(chunks):

        def down(b):
            part = jnp.dot(
                hidden[b], wd[:, j * cols : (j + 1) * cols], preferred_element_type=jnp.float32
            )
            p_own[j, b] = part[:block].astype(jnp.bfloat16)
            p_send[j, b] = part[block:].astype(jnp.bfloat16)

        loop(blocks, down)
        to_sib(p_send, p_recv, j, q_send, q_recv).start()

    for j in range(chunks):
        to_sib(p_send, p_recv, j, q_send, q_recv).wait_recv()

        def combine(b):
            total = p_own[j, b].astype(jnp.float32) + p_recv[j, b].astype(jnp.float32)
            pack(total, c_send, j, b)

        loop(blocks, combine)
        exchange(c_send, c_recv, j, b_send, b_recv)

    spread = w_rows[...].T
    high = spread.astype(jnp.bfloat16)
    low = (spread - high.astype(jnp.float32)).astype(jnp.bfloat16)
    for j in range(chunks):
        all_of(c_send, c_recv, j, b_send, b_recv).wait_recv()

        def unpack(b):
            got = c_recv[j, pl.ds(b * block, block)].astype(jnp.float32)
            flat[: block * SUB, :] = got.reshape(block * SUB, LANES)
            at = start_of(b)
            for s in range(SUB):
                r_cols[pl.ds(at, block), s * LANES : (s + 1) * LANES] = flat[
                    pl.ds(s, block, stride=SUB), :
                ]

        loop(blocks, unpack)
        res = r_cols[...].astype(jnp.bfloat16)
        total = jnp.dot(high, res, preferred_element_type=jnp.float32)
        total = total + jnp.dot(low, res, preferred_element_type=jnp.float32)
        mixed[:, j * cols : (j + 1) * cols] = total.astype(jnp.bfloat16)

    for j in range(chunks):
        all_of(out_x, in_x, j, d_send, d_recv).wait_send()
        to_sib(in_x, sib_x, j, f_send, f_recv).wait_send()
        to_sib(p_send, p_recv, j, q_send, q_recv).wait_send()
        all_of(c_send, c_recv, j, b_send, b_recv).wait_send()


def local(n, tokens, norm_gain, chosen_rows, route_weights, gate_weight, up_weight, down_weight):
    tok_rows, width = tokens.shape
    half_rows = tok_rows // 2
    experts, slots = chosen_rows.shape
    half = slots // 2
    rows = experts * half
    block = GROUP * half
    blocks = rows // block
    ff = gate_weight.shape[2]
    chunks = width // (LANES * SUB)
    cols = width // chunks
    bf16, f32 = jnp.bfloat16, jnp.float32
    packed = pltpu.VMEM((chunks, rows, SUB, LANES), bf16)
    partial = pltpu.VMEM((chunks, blocks, block, cols), bf16)
    vmem = pl.BlockSpec(memory_space=pltpu.VMEM)
    hbm = pl.BlockSpec(memory_space=pltpu.HBM)
    scratch = [
        pltpu.VMEM((half_rows, width), bf16),
        pltpu.VMEM(norm_gain.shape, norm_gain.dtype),
        pltpu.VMEM(chosen_rows.shape, chosen_rows.dtype),
        pltpu.VMEM(route_weights.shape, route_weights.dtype),
        pltpu.VMEM(gate_weight.shape[1:], bf16),
        pltpu.VMEM(up_weight.shape[1:], bf16),
        pltpu.VMEM(down_weight.shape[1:], bf16),
        pltpu.VMEM((half_rows, width), bf16),
        packed,
        packed,
        packed,
        pltpu.VMEM((2 * block * SUB, LANES), f32),
        pltpu.VMEM((2 * block, cols), bf16),
        pltpu.VMEM((blocks, 2 * block, ff), f32),
        pltpu.VMEM((blocks, 2 * block, ff), f32),
        pltpu.VMEM((blocks, 2 * block, ff), bf16),
        partial,
        partial,
        partial,
        packed,
        packed,
        pltpu.VMEM((rows, half_rows), f32),
        pltpu.VMEM((rows, half_rows), f32),
        pltpu.VMEM((rows, cols), f32),
    ]
    limit = VMEM_BYTES - half_rows * width * 2
    return pl.pallas_call(
        functools.partial(kernel, n),
        out_shape=pltpu.VMEM((half_rows, width), bf16),
        in_specs=[hbm] * 7,
        out_specs=vmem,
        scratch_shapes=scratch
        + [pltpu.SemaphoreType.DMA((7,))]
        + [pltpu.SemaphoreType.DMA((chunks,))] * 8,
        compiler_params=pltpu.CompilerParams(
            collective_id=0, has_side_effects=True, vmem_limit_bytes=limit
        ),
    )(
        tokens,
        norm_gain,
        chosen_rows,
        route_weights,
        gate_weight,
        up_weight,
        down_weight,
    )


def solution(mesh):
    return jax.shard_map(
        functools.partial(local, mesh.shape["ep"]),
        mesh=mesh,
        in_specs=(
            P(("grp", "ep"), None),
            P(),
            P("grp", "ep"),
            P("grp", "ep"),
            P("ep", None, "tp"),
            P("ep", None, "tp"),
            P("ep", "tp", None),
        ),
        out_specs=P(("grp", "ep", "tp"), None),
        check_vma=False,
    )
```

```python
import functools

import jax
import jax.numpy as jnp
from jax import lax
from jax.experimental import pallas as pl
from jax.experimental.pallas import tpu as pltpu
from jax.sharding import PartitionSpec as P

MESH = pl.DeviceIdType.MESH
LANES = 128
SUB = 8
GROUP = 8
VMEM_BYTES = 67043328


def loop(count, body):
    if count == 1:
        body(0)
    else:
        lax.fori_loop(0, count, lambda i, carry: (body(i), carry)[1], 0)


def group_sizes(half):
    return [half - half // 2, half // 2]


def kernel(
    n,
    tokens,
    gain_h,
    chosen_h,
    route_h,
    gate_w,
    up_w,
    down_w,
    mixed,
    tok,
    gain,
    chosen,
    route,
    wg,
    wu,
    wd,
    normed,
    out_x,
    in_x,
    sib_x,
    flat,
    x_cols,
    hidden,
    p_send,
    p_recv,
    p_own,
    c_send,
    c_recv,
    g_rows,
    w_rows,
    r_cols,
    load_sem,
    d_send,
    d_recv,
    f_send,
    f_recv,
    q_send,
    q_recv,
    b_send,
    b_recv,
):
    half_rows, width = tok.shape
    experts, slots = chosen.shape
    half = slots // 2
    sizes = group_sizes(half)
    starts = [sum(sizes[:j]) for j in range(len(sizes))]
    blocks = experts // GROUP
    pieces = width // LANES
    cols = width // 2
    me = lax.axis_index("ep")
    core = lax.axis_index("tp")
    sib = {"tp": 1 - core}

    def peer(i):
        return lax.rem(me + i, n)

    barrier = pltpu.get_barrier_semaphore()
    pl.semaphore_signal(barrier, inc=1, device_id=sib, device_id_type=MESH)
    lax.fori_loop(
        1,
        n,
        lambda i, c: (
            pl.semaphore_signal(barrier, inc=1, device_id={"ep": peer(i)}, device_id_type=MESH),
            c,
        )[1],
        0,
    )
    base = pl.multiple_of(core * half_rows, 8)
    load_tok = pltpu.make_async_copy(tokens.at[pl.ds(base, half_rows)], tok, load_sem.at[0])
    load_tok.start()
    small = [
        pltpu.make_async_copy(src, dst, load_sem.at[i + 4])
        for i, (src, dst) in enumerate(((gain_h, gain), (chosen_h, chosen), (route_h, route)))
    ]
    for load in small:
        load.start()
    loads = [
        pltpu.make_async_copy(src.at[0], dst, load_sem.at[i + 1])
        for i, (src, dst) in enumerate(((gate_w, wg), (up_w, wu), (down_w, wd)))
    ]
    for load in small:
        load.wait()
    first = me * (2 * half_rows) + core * half_rows
    picked = (chosen[...] - first).astype(jnp.float32).T
    weight = route[...].T
    lane = lax.broadcasted_iota(jnp.int32, (half, half_rows), 1).astype(jnp.float32)
    for e in range(experts):
        pair = [picked[h * half : (h + 1) * half, e : e + 1] for h in range(2)]
        row = jnp.where(core == 0, pair[0], pair[1])
        pair = [weight[h * half : (h + 1) * half, e : e + 1] for h in range(2)]
        share = jnp.where(core == 0, pair[0], pair[1])
        here = lane == row
        for j, size in enumerate(sizes):
            here_j = slice(starts[j], starts[j] + size)
            at = slice(experts * starts[j] + e * size, experts * starts[j] + (e + 1) * size)
            g_rows[at, :] = jnp.where(here, 1.0, 0.0)[here_j]
            w_rows[at, :] = jnp.where(here, share, 0.0)[here_j]

    load_tok.wait()
    for load in loads:
        load.start()

    g = gain[...].astype(jnp.float32).reshape(1, width)
    values = tok[...].astype(jnp.float32)
    scale = lax.rsqrt(jnp.mean(values * values, axis=-1, keepdims=True) + 1e-06)
    normed[...] = (values * scale * g).astype(jnp.bfloat16)

    def rows_of(j, b):
        block = GROUP * sizes[j]
        at = b * block
        return pl.ds(at if isinstance(b, int) else pl.multiple_of(at, 8), block)

    def total_rows(j, b):
        block = GROUP * sizes[j]
        at = experts * starts[j] + b * block
        return pl.ds(at if isinstance(b, int) else pl.multiple_of(at, 8), block)

    def pack(value, ref, j, b):
        block = GROUP * sizes[j]
        for s in range(pieces):
            flat[pl.ds(s, block, stride=pieces), :] = value[:, s * LANES : (s + 1) * LANES]
        packed = flat[: block * pieces, :].reshape(block, pieces, LANES)
        ref[j, rows_of(j, b)] = packed.astype(jnp.bfloat16)

    def gather(j):
        def one(b):
            hot = g_rows[total_rows(j, b), :].astype(jnp.bfloat16)
            got = jnp.dot(hot, normed[...], preferred_element_type=jnp.float32)
            pack(got, out_x, j, b)

        loop(blocks, one)

    def mine(ref, j, e):
        return ref.at[j, pl.ds(e * sizes[j], sizes[j])]

    def exchange(src, dst, j, send_sem, recv_sem):
        def one(i, c):
            e = peer(i)
            pltpu.make_async_remote_copy(
                src_ref=mine(src, j, e),
                dst_ref=mine(dst, j, me),
                send_sem=send_sem.at[j],
                recv_sem=recv_sem.at[j],
                device_id={"ep": e},
                device_id_type=MESH,
            ).start()
            return c

        lax.fori_loop(1, n, one, 0)
        for r in range(sizes[j]):
            dst[j, me * sizes[j] + r] = src[j, me * sizes[j] + r]

    def all_of(src, dst, j, send_sem, recv_sem):
        part = pl.ds(0, (n - 1) * sizes[j])
        return pltpu.make_async_remote_copy(
            src_ref=src.at[j, part],
            dst_ref=dst.at[j, part],
            send_sem=send_sem.at[j],
            recv_sem=recv_sem.at[j],
            device_id=sib,
            device_id_type=MESH,
        )

    def forward(j):
        part = pl.ds(0, n * sizes[j])
        return pltpu.make_async_remote_copy(
            src_ref=in_x.at[j, part],
            dst_ref=sib_x.at[j, part],
            send_sem=f_send.at[j],
            recv_sem=f_recv.at[j],
            device_id=sib,
            device_id_type=MESH,
        )

    def swap(j, k):
        part = pl.ds(0, n * sizes[j])
        return pltpu.make_async_remote_copy(
            src_ref=p_send.at[j, k, part],
            dst_ref=p_recv.at[j, k, part],
            send_sem=q_send.at[2 * j + k],
            recv_sem=q_recv.at[2 * j + k],
            device_id=sib,
            device_id_type=MESH,
        )

    groups = range(len(sizes))
    gather(0)
    pl.semaphore_wait(barrier, n)
    exchange(out_x, in_x, 0, d_send, d_recv)
    for j in groups[1:]:
        gather(j)
        exchange(out_x, in_x, j, d_send, d_recv)

    def arrive(j):
        all_of(out_x, in_x, j, d_send, d_recv).wait_recv()
        forward(j).start()

    def compute(j):
        block = GROUP * sizes[j]

        def project(b):
            for h, ref in enumerate((in_x, sib_x)):
                got = ref[j, rows_of(j, b)].astype(jnp.float32)
                flat[pl.ds(h * block * pieces, block * pieces), :] = got.reshape(
                    block * pieces, LANES
                )
            for s in range(pieces):
                x_cols[: 2 * block, s * LANES : (s + 1) * LANES] = flat[
                    pl.ds(s, 2 * block, stride=pieces), :
                ].astype(jnp.bfloat16)
            x = x_cols[: 2 * block, :]
            gate = jnp.dot(x, wg[...], preferred_element_type=jnp.float32)
            up = jnp.dot(x, wu[...], preferred_element_type=jnp.float32)
            act = (gate / (1.0 + jnp.exp(-gate)) * up).astype(jnp.bfloat16)
            hidden[b, : 2 * block, :] = act

        loop(blocks, project)
        if j == 0:
            loads[2].wait()
        for k in range(2):

            def down(b):
                part = jnp.dot(
                    hidden[b, : 2 * block, :],
                    wd[:, k * cols : (k + 1) * cols],
                    preferred_element_type=jnp.float32,
                )
                p_own[j, k, rows_of(j, b)] = part[:block].astype(jnp.bfloat16)
                p_send[j, k, rows_of(j, b)] = part[block:].astype(jnp.bfloat16)

            loop(blocks, down)
            swap(j, k).start()

    def give(j):
        for k in range(2):
            swap(j, k).wait_recv()

        def combine(b):
            both = [
                p_own[j, k, rows_of(j, b)].astype(jnp.float32)
                + p_recv[j, k, rows_of(j, b)].astype(jnp.float32)
                for k in range(2)
            ]
            pack(jnp.concatenate(both, axis=1), c_send, j, b)

        loop(blocks, combine)
        exchange(c_send, c_recv, j, b_send, b_recv)

    arrive(0)
    for load in loads[:2]:
        load.wait()
    for j in groups:
        forward(j).wait_recv()
        compute(j)
        if j + 1 < len(sizes):
            arrive(j + 1)
        give(j)

    spread = w_rows[...].T
    high = spread.astype(jnp.bfloat16)
    low = (spread - high.astype(jnp.float32)).astype(jnp.bfloat16)
    for j in groups:
        all_of(c_send, c_recv, j, b_send, b_recv).wait_recv()
        block = GROUP * sizes[j]

        def unpack(b):
            got = c_recv[j, rows_of(j, b)].astype(jnp.float32)
            flat[: block * pieces, :] = got.reshape(block * pieces, LANES)
            for s in range(pieces):
                r_cols[total_rows(j, b), s * LANES : (s + 1) * LANES] = flat[
                    pl.ds(s, block, stride=pieces), :
                ]

        loop(blocks, unpack)
    for k in range(2):
        part = slice(k * cols, (k + 1) * cols)
        res = r_cols[:, part].astype(jnp.bfloat16)
        total = jnp.dot(high, res, preferred_element_type=jnp.float32)
        total = total + jnp.dot(low, res, preferred_element_type=jnp.float32)
        mixed[:, part] = total.astype(jnp.bfloat16)

    for j in groups:
        all_of(out_x, in_x, j, d_send, d_recv).wait_send()
        forward(j).wait_send()
        for k in range(2):
            swap(j, k).wait_send()
        all_of(c_send, c_recv, j, b_send, b_recv).wait_send()


def local(n, tokens, norm_gain, chosen_rows, route_weights, gate_weight, up_weight, down_weight):
    tok_rows, width = tokens.shape
    half_rows = tok_rows // 2
    experts, slots = chosen_rows.shape
    half = slots // 2
    rows = experts * half
    sizes = group_sizes(half)
    top = max(sizes)
    block = GROUP * top
    pieces = width // LANES
    ff = gate_weight.shape[2]
    bf16, f32 = jnp.bfloat16, jnp.float32
    packed = pltpu.VMEM((len(sizes), experts * top, pieces, LANES), bf16)
    partial = pltpu.VMEM((len(sizes), 2, experts * top, width // 2), bf16)
    vmem = pl.BlockSpec(memory_space=pltpu.VMEM)
    hbm = pl.BlockSpec(memory_space=pltpu.HBM)
    scratch = [
        pltpu.VMEM((half_rows, width), bf16),
        pltpu.VMEM(norm_gain.shape, norm_gain.dtype),
        pltpu.VMEM(chosen_rows.shape, chosen_rows.dtype),
        pltpu.VMEM(route_weights.shape, route_weights.dtype),
        pltpu.VMEM(gate_weight.shape[1:], bf16),
        pltpu.VMEM(up_weight.shape[1:], bf16),
        pltpu.VMEM(down_weight.shape[1:], bf16),
        pltpu.VMEM((half_rows, width), bf16),
        packed,
        packed,
        packed,
        pltpu.VMEM((2 * block * pieces, LANES), f32),
        pltpu.VMEM((2 * block, width), bf16),
        pltpu.VMEM((experts // GROUP, 2 * block, ff), bf16),
        partial,
        partial,
        partial,
        packed,
        packed,
        pltpu.VMEM((rows, half_rows), f32),
        pltpu.VMEM((rows, half_rows), f32),
        pltpu.VMEM((rows, width), f32),
    ]
    limit = VMEM_BYTES - half_rows * width * 2
    return pl.pallas_call(
        functools.partial(kernel, n),
        out_shape=pltpu.VMEM((half_rows, width), bf16),
        in_specs=[hbm] * 7,
        out_specs=vmem,
        scratch_shapes=scratch
        + [pltpu.SemaphoreType.DMA((7,))]
        + [pltpu.SemaphoreType.DMA((2 * len(sizes),))] * 8,
        compiler_params=pltpu.CompilerParams(
            collective_id=0, has_side_effects=True, vmem_limit_bytes=limit
        ),
    )(
        tokens,
        norm_gain,
        chosen_rows,
        route_weights,
        gate_weight,
        up_weight,
        down_weight,
    )


def solution(mesh):
    return jax.shard_map(
        functools.partial(local, mesh.shape["ep"]),
        mesh=mesh,
        in_specs=(
            P(("grp", "ep"), None),
            P(),
            P("grp", "ep"),
            P("grp", "ep"),
            P("ep", None, "tp"),
            P("ep", None, "tp"),
            P("ep", "tp", None),
        ),
        out_specs=P(("grp", "ep", "tp"), None),
        check_vma=False,
    )
```

```python
import functools

import jax
import jax.numpy as jnp
from jax import lax
from jax.experimental import pallas as pl
from jax.experimental.pallas import tpu as pltpu
from jax.sharding import PartitionSpec as P

MESH = pl.DeviceIdType.MESH
LANES = 128
SUB = 8
GROUP = 8
VMEM_BYTES = 67043328


def loop(count, body):
    if count == 1:
        body(0)
    else:
        lax.fori_loop(0, count, lambda i, carry: (body(i), carry)[1], 0)


def group_sizes(half):
    return [half // 2, half - half // 2]


def kernel(
    n,
    tokens,
    gain_h,
    chosen_h,
    route_h,
    gate_w,
    up_w,
    down_w,
    mixed,
    tok,
    gain,
    chosen,
    route,
    wg,
    wu,
    wd,
    normed,
    out_x,
    in_x,
    sib_x,
    flat,
    x_cols,
    hidden,
    p_send,
    p_recv,
    p_own,
    c_send,
    c_recv,
    g_rows,
    w_rows,
    r_cols,
    load_sem,
    d_send,
    d_recv,
    f_send,
    f_recv,
    q_send,
    q_recv,
    b_send,
    b_recv,
):
    half_rows, width = tok.shape
    experts, slots = chosen.shape
    half = slots // 2
    sizes = group_sizes(half)
    starts = [sum(sizes[:j]) for j in range(len(sizes))]
    blocks = experts // GROUP
    pieces = width // LANES
    cols = width // 2
    me = lax.axis_index("ep")
    core = lax.axis_index("tp")
    sib = {"tp": 1 - core}

    def peer(i):
        return lax.rem(me + i, n)

    barrier = pltpu.get_barrier_semaphore()
    pl.semaphore_signal(barrier, inc=1, device_id=sib, device_id_type=MESH)
    lax.fori_loop(
        1,
        n,
        lambda i, c: (
            pl.semaphore_signal(barrier, inc=1, device_id={"ep": peer(i)}, device_id_type=MESH),
            c,
        )[1],
        0,
    )
    base = pl.multiple_of(core * half_rows, 8)
    load_tok = pltpu.make_async_copy(tokens.at[pl.ds(base, half_rows)], tok, load_sem.at[0])
    load_tok.start()
    small = [
        pltpu.make_async_copy(src, dst, load_sem.at[i + 4])
        for i, (src, dst) in enumerate(((gain_h, gain), (chosen_h, chosen), (route_h, route)))
    ]
    for load in small:
        load.start()
    loads = [
        pltpu.make_async_copy(src.at[0], dst, load_sem.at[i + 1])
        for i, (src, dst) in enumerate(((gate_w, wg), (up_w, wu), (down_w, wd)))
    ]
    for load in small:
        load.wait()
    first = me * (2 * half_rows) + core * half_rows
    picked = (chosen[...] - first).astype(jnp.float32).T
    weight = route[...].T
    lane = lax.broadcasted_iota(jnp.int32, (half, half_rows), 1).astype(jnp.float32)
    for e in range(experts):
        pair = [picked[h * half : (h + 1) * half, e : e + 1] for h in range(2)]
        row = jnp.where(core == 0, pair[0], pair[1])
        pair = [weight[h * half : (h + 1) * half, e : e + 1] for h in range(2)]
        share = jnp.where(core == 0, pair[0], pair[1])
        here = lane == row
        for j, size in enumerate(sizes):
            here_j = slice(starts[j], starts[j] + size)
            at = slice(experts * starts[j] + e * size, experts * starts[j] + (e + 1) * size)
            g_rows[at, :] = jnp.where(here, 1.0, 0.0)[here_j]
            w_rows[at, :] = jnp.where(here, share, 0.0)[here_j]

    load_tok.wait()
    for load in loads:
        load.start()

    g = gain[...].astype(jnp.float32).reshape(1, width)
    values = tok[...].astype(jnp.float32)
    scale = lax.rsqrt(jnp.mean(values * values, axis=-1, keepdims=True) + 1e-06)
    normed[...] = (values * scale * g).astype(jnp.bfloat16)

    def rows_of(j, b):
        block = GROUP * sizes[j]
        at = b * block
        return pl.ds(at if isinstance(b, int) else pl.multiple_of(at, 8), block)

    def total_rows(j, b):
        block = GROUP * sizes[j]
        at = experts * starts[j] + b * block
        return pl.ds(at if isinstance(b, int) else pl.multiple_of(at, 8), block)

    def pack(value, ref, j, b):
        block = GROUP * sizes[j]
        for s in range(pieces):
            flat[pl.ds(s, block, stride=pieces), :] = value[:, s * LANES : (s + 1) * LANES]
        packed = flat[: block * pieces, :].reshape(block, pieces, LANES)
        ref[j, rows_of(j, b)] = packed.astype(jnp.bfloat16)

    def gather(j):
        def one(b):
            hot = g_rows[total_rows(j, b), :].astype(jnp.bfloat16)
            got = jnp.dot(hot, normed[...], preferred_element_type=jnp.float32)
            pack(got, out_x, j, b)

        loop(blocks, one)

    def mine(ref, j, e):
        return ref.at[j, pl.ds(e * sizes[j], sizes[j])]

    def exchange(src, dst, j, send_sem, recv_sem):
        def one(i, c):
            e = peer(i)
            pltpu.make_async_remote_copy(
                src_ref=mine(src, j, e),
                dst_ref=mine(dst, j, me),
                send_sem=send_sem.at[j],
                recv_sem=recv_sem.at[j],
                device_id={"ep": e},
                device_id_type=MESH,
            ).start()
            return c

        lax.fori_loop(1, n, one, 0)
        for r in range(sizes[j]):
            dst[j, me * sizes[j] + r] = src[j, me * sizes[j] + r]

    def all_of(src, dst, j, send_sem, recv_sem):
        part = pl.ds(0, (n - 1) * sizes[j])
        return pltpu.make_async_remote_copy(
            src_ref=src.at[j, part],
            dst_ref=dst.at[j, part],
            send_sem=send_sem.at[j],
            recv_sem=recv_sem.at[j],
            device_id=sib,
            device_id_type=MESH,
        )

    def forward(j):
        part = pl.ds(0, n * sizes[j])
        return pltpu.make_async_remote_copy(
            src_ref=in_x.at[j, part],
            dst_ref=sib_x.at[j, part],
            send_sem=f_send.at[j],
            recv_sem=f_recv.at[j],
            device_id=sib,
            device_id_type=MESH,
        )

    def swap(j, k):
        part = pl.ds(0, n * sizes[j])
        return pltpu.make_async_remote_copy(
            src_ref=p_send.at[j, k, part],
            dst_ref=p_recv.at[j, k, part],
            send_sem=q_send.at[2 * j + k],
            recv_sem=q_recv.at[2 * j + k],
            device_id=sib,
            device_id_type=MESH,
        )

    groups = range(len(sizes))
    gather(0)
    pl.semaphore_wait(barrier, n)
    exchange(out_x, in_x, 0, d_send, d_recv)
    for j in groups[1:]:
        gather(j)
        exchange(out_x, in_x, j, d_send, d_recv)

    def arrive(j):
        all_of(out_x, in_x, j, d_send, d_recv).wait_recv()
        forward(j).start()

    def compute(j):
        block = GROUP * sizes[j]

        def project(b):
            for h, ref in enumerate((in_x, sib_x)):
                got = ref[j, rows_of(j, b)].astype(jnp.float32)
                flat[pl.ds(h * block * pieces, block * pieces), :] = got.reshape(
                    block * pieces, LANES
                )
            for s in range(pieces):
                x_cols[: 2 * block, s * LANES : (s + 1) * LANES] = flat[
                    pl.ds(s, 2 * block, stride=pieces), :
                ].astype(jnp.bfloat16)
            x = x_cols[: 2 * block, :]
            gate = jnp.dot(x, wg[...], preferred_element_type=jnp.float32)
            up = jnp.dot(x, wu[...], preferred_element_type=jnp.float32)
            act = (gate / (1.0 + jnp.exp(-gate)) * up).astype(jnp.bfloat16)
            hidden[b, : 2 * block, :] = act

        loop(blocks, project)
        if j == 0:
            loads[2].wait()
        for k in range(2):

            def down(b):
                part = jnp.dot(
                    hidden[b, : 2 * block, :],
                    wd[:, k * cols : (k + 1) * cols],
                    preferred_element_type=jnp.float32,
                )
                p_own[j, k, rows_of(j, b)] = part[:block].astype(jnp.bfloat16)
                p_send[j, k, rows_of(j, b)] = part[block:].astype(jnp.bfloat16)

            loop(blocks, down)
            swap(j, k).start()

    def give(j):
        for k in range(2):
            swap(j, k).wait_recv()

        def combine(b):
            both = [
                p_own[j, k, rows_of(j, b)].astype(jnp.float32)
                + p_recv[j, k, rows_of(j, b)].astype(jnp.float32)
                for k in range(2)
            ]
            pack(jnp.concatenate(both, axis=1), c_send, j, b)

        loop(blocks, combine)
        exchange(c_send, c_recv, j, b_send, b_recv)

    arrive(0)
    for load in loads[:2]:
        load.wait()
    for j in groups:
        forward(j).wait_recv()
        compute(j)
        if j + 1 < len(sizes):
            arrive(j + 1)
        give(j)

    spread = w_rows[...].T
    high = spread.astype(jnp.bfloat16)
    low = (spread - high.astype(jnp.float32)).astype(jnp.bfloat16)
    for j in groups:
        all_of(c_send, c_recv, j, b_send, b_recv).wait_recv()
        block = GROUP * sizes[j]

        def unpack(b):
            got = c_recv[j, rows_of(j, b)].astype(jnp.float32)
            flat[: block * pieces, :] = got.reshape(block * pieces, LANES)
            for s in range(pieces):
                r_cols[total_rows(j, b), s * LANES : (s + 1) * LANES] = flat[
                    pl.ds(s, block, stride=pieces), :
                ]

        loop(blocks, unpack)
    for k in range(2):
        part = slice(k * cols, (k + 1) * cols)
        res = r_cols[:, part].astype(jnp.bfloat16)
        total = jnp.dot(high, res, preferred_element_type=jnp.float32)
        total = total + jnp.dot(low, res, preferred_element_type=jnp.float32)
        mixed[:, part] = total.astype(jnp.bfloat16)

    for j in groups:
        all_of(out_x, in_x, j, d_send, d_recv).wait_send()
        forward(j).wait_send()
        for k in range(2):
            swap(j, k).wait_send()
        all_of(c_send, c_recv, j, b_send, b_recv).wait_send()


def local(n, tokens, norm_gain, chosen_rows, route_weights, gate_weight, up_weight, down_weight):
    tok_rows, width = tokens.shape
    half_rows = tok_rows // 2
    experts, slots = chosen_rows.shape
    half = slots // 2
    rows = experts * half
    sizes = group_sizes(half)
    top = max(sizes)
    block = GROUP * top
    pieces = width // LANES
    ff = gate_weight.shape[2]
    bf16, f32 = jnp.bfloat16, jnp.float32
    packed = pltpu.VMEM((len(sizes), experts * top, pieces, LANES), bf16)
    partial = pltpu.VMEM((len(sizes), 2, experts * top, width // 2), bf16)
    vmem = pl.BlockSpec(memory_space=pltpu.VMEM)
    hbm = pl.BlockSpec(memory_space=pltpu.HBM)
    scratch = [
        pltpu.VMEM((half_rows, width), bf16),
        pltpu.VMEM(norm_gain.shape, norm_gain.dtype),
        pltpu.VMEM(chosen_rows.shape, chosen_rows.dtype),
        pltpu.VMEM(route_weights.shape, route_weights.dtype),
        pltpu.VMEM(gate_weight.shape[1:], bf16),
        pltpu.VMEM(up_weight.shape[1:], bf16),
        pltpu.VMEM(down_weight.shape[1:], bf16),
        pltpu.VMEM((half_rows, width), bf16),
        packed,
        packed,
        packed,
        pltpu.VMEM((2 * block * pieces, LANES), f32),
        pltpu.VMEM((2 * block, width), bf16),
        pltpu.VMEM((experts // GROUP, 2 * block, ff), bf16),
        partial,
        partial,
        partial,
        packed,
        packed,
        pltpu.VMEM((rows, half_rows), f32),
        pltpu.VMEM((rows, half_rows), f32),
        pltpu.VMEM((rows, width), f32),
    ]
    limit = VMEM_BYTES - half_rows * width * 2
    return pl.pallas_call(
        functools.partial(kernel, n),
        out_shape=pltpu.VMEM((half_rows, width), bf16),
        in_specs=[hbm] * 7,
        out_specs=vmem,
        scratch_shapes=scratch
        + [pltpu.SemaphoreType.DMA((7,))]
        + [pltpu.SemaphoreType.DMA((2 * len(sizes),))] * 8,
        compiler_params=pltpu.CompilerParams(
            collective_id=0, has_side_effects=True, vmem_limit_bytes=limit
        ),
    )(
        tokens,
        norm_gain,
        chosen_rows,
        route_weights,
        gate_weight,
        up_weight,
        down_weight,
    )


def solution(mesh):
    return jax.shard_map(
        functools.partial(local, mesh.shape["ep"]),
        mesh=mesh,
        in_specs=(
            P(("grp", "ep"), None),
            P(),
            P("grp", "ep"),
            P("grp", "ep"),
            P("ep", None, "tp"),
            P("ep", None, "tp"),
            P("ep", "tp", None),
        ),
        out_specs=P(("grp", "ep", "tp"), None),
        check_vma=False,
    )
```
